32 devices in a mesh: grp: 2 (over x), ep: 16 (over z, y, core).
Axes of the slice: x: 2, y: 2, z: 4, core: 2. Of those that a mesh axis runs over, the one named last changes fastest.
Arguments:
- hidden: bfloat16 [4096, 2048], P(('grp', 'ep')), parts along dimension 0, may hold values from -6 to 6
- state: float32 [2, 4096, 4096], P(None, ('grp', 'ep')), parts along dimension 1, may hold values from -6 to 6
- norm_gain: float32 [2048], replicated, may hold values from 0.1 to 1.9
- w_in: bfloat16 [2048, 1024], P(None, 'ep'), may hold values from -0.125 to 0.125
- lam_re: float32 [64, 64], replicated, may hold values from -1 to -0.1
- lam_im: float32 [64, 64], replicated, may hold values from 0 to 200
- log_step: float32 [64], replicated, may hold values from -4.6 to -0.7
- in_re: float32 [64, 64, 16], replicated, may hold values from -1 to 1
- in_im: float32 [64, 64, 16], replicated, may hold values from -1 to 1
- out_re: float32 [64, 16, 64], replicated, may hold values from -0.75 to 0.75
- out_im: float32 [64, 16, 64], replicated, may hold values from -0.75 to 0.75
- skip: float32 [1024], replicated, may hold values from -4 to 4
- w_glu: bfloat16 [1024, 1024], replicated, may hold values from -0.1875 to 0.1875
- w_out: bfloat16 [1024, 2048], replicated, may hold values from -0.375 to 0.375
- ffn_gain: float32 [2048], replicated, may hold values from 0.1 to 1.9
- w_group: bfloat16 [2048, 4], replicated, may hold values from -0.03125 to 0.03125
- w_route: bfloat16 [2048, 16], replicated, may hold values from -0.03125 to 0.03125
- w_gate: bfloat16 [16, 2048, 512], P('ep'), may hold values from -0.125 to 0.125
- w_up: bfloat16 [16, 2048, 512], P('ep'), may hold values from -0.125 to 0.125
- w_down: bfloat16 [16, 512, 2048], P('ep'), may hold values from -2 to 2
- route_ids: int32 [4096, 2], P(('grp', 'ep')), parts along dimension 0, may hold values from 0 to 15, as said below
Outputs:
- hidden_out: bfloat16 [4096, 2048], P(('grp', 'ep')), parts along dimension 0
- new_state: float32 [2, 4096, 4096], P(None, ('grp', 'ep')), parts along dimension 1
The draws below stay inside these ranges and needn't reach their ends.
There are 2 independent parts, one for each index of `grp`. The reference program is written for one: setup_inputs(seed, part) draws one part's arguments, and reference() takes and returns one part's arrays. A program takes and returns all parts, laid end to end along the dimension named above; an argument that names none is the same for every part. Nothing has to cross between parts.
Inputs may be any that keep to these rules, and one draw needn't show every extreme that they name: `route_ids`: each row names 2 different experts of one expert group (experts g * 4 to g * 4 + 3). Among the rows of one device no expert is named more than 32 times, and in every draw some experts are named exactly 32 times by the rows of every device.
All inputs are finite; a program needn't handle non-finite values.
Results may differ from the reference program's by a relative error of at most 0.013.
Values may be sent and summed in bfloat16 or wider, within the bound.
No kernel may reach another device: no remote copies, remote signals or barrier semaphores. Data moves between devices by JAX's collectives and lax.ppermute only.
A program may use at most 128 MiB of HBM per device.

```python
import jax
import jax.numpy as jnp
from jax import lax

D = 2048
S5W = 1024
GROUP_CH = 16
STATE = 64
FFE = 512
EXP_GROUPS = 4
TOPK = 2
SEQ_DEV = 128
SEQS = 2048
EXPERTS = 16
EPG = 4
CAP = 32
GROUPS_S5 = 64
N_EP = 16


def draw_route_ids(key, part):
    base = jax.random.fold_in(key, 11)
    big_key, rest_key = jax.random.split(base)
    big = jax.random.randint(big_key, (), 0, EXP_GROUPS)
    half = SEQ_DEV // 2

    def one_block(block_key):
        order_key, other_key, shift_key, label_key = jax.random.split(block_key, 4)
        order = jax.random.permutation(order_key, SEQ_DEV)
        others = (big + 1 + jax.random.randint(other_key, (SEQ_DEV,), 0, EXP_GROUPS - 1)) % EXP_GROUPS
        by_place = jnp.where(jnp.arange(SEQ_DEV) < half, big, others).astype(jnp.int32)
        group = jnp.zeros((SEQ_DEV,), jnp.int32).at[order].set(by_place)
        member = (group[:, None] == jnp.arange(EXP_GROUPS, dtype=jnp.int32)[None, :]).astype(jnp.int32)
        rank = jnp.sum((jnp.cumsum(member, axis=0) - member) * member, axis=1)
        shift = jax.random.randint(shift_key, (EXP_GROUPS,), 0, EPG)
        labels = jax.vmap(lambda sub: jax.random.permutation(sub, EPG))(jax.random.split(label_key, EXP_GROUPS))
        first = (2 * rank + shift[group]) % EPG
        second = (2 * rank + 1 + shift[group]) % EPG
        one = group * EPG + labels[group, first]
        two = group * EPG + labels[group, second]
        return jnp.stack([one, two], axis=1).astype(jnp.int32)
    blocks = jax.vmap(one_block)(jax.random.split(rest_key, SEQS // SEQ_DEV))
    return blocks.reshape(SEQS, TOPK)


def block_scale(stream_key, extent, cuts, low, top_value):
    def one(axis_at, parts):
        draws = jax.random.uniform(jax.random.fold_in(jax.random.fold_in(stream_key, 6), axis_at), (parts,), jnp.float32, low / len(cuts), top_value / len(cuts))
        return jnp.repeat(jnp.exp(draws), extent[axis_at] // parts).reshape((-1,) + (1,) * (len(extent) - axis_at - 1))

    level = one(*cuts[0])
    for cut in cuts[1:]:
        level = level * one(*cut)
    return level


def gaussian(own_key, extent, scale, most, pieces=(), held_as=jnp.bfloat16):
    array = scale * jax.random.normal(own_key, extent, jnp.float32)
    if pieces:
        array = array * block_scale(own_key, extent, pieces, -0.22, 0.18)
    return jnp.clip(array, -most, most).astype(held_as)


def setup_inputs(seed: int = 0, part: int = 0) -> dict:
    key_list = jax.random.split(jax.random.key(seed), 22)
    own_keys = jax.random.split(jax.random.fold_in(key_list[21], part), 22)
    hidden = gaussian(own_keys[0], (SEQS, D), 1.0, 6.0, ((0, 16),))
    state = gaussian(own_keys[1], (2, SEQS, GROUPS_S5 * STATE), 1.0, 6.0, ((1, 16),), jnp.float32)
    norm_gain = jnp.clip(1.0 + 0.18 * jax.random.normal(key_list[2], (D,), jnp.float32), 0.1, 1.9)
    w_in = gaussian(key_list[3], (D, S5W), D ** -0.5, 0.125, ((1, 16),))
    lam_re = jnp.clip(jax.random.uniform(key_list[4], (GROUPS_S5, STATE), jnp.float32, -1.0, -0.1), -1.0, -0.1)
    lam_im = jnp.clip(jax.random.uniform(key_list[5], (GROUPS_S5, STATE), jnp.float32, 0.0, 200.0), 0.0, 200.0)
    log_step = jnp.clip(jax.random.uniform(key_list[6], (GROUPS_S5,), jnp.float32, -4.6, -0.7), -4.6, -0.7)
    in_re = gaussian(key_list[7], (GROUPS_S5, STATE, GROUP_CH), (2 * GROUP_CH) ** -0.5, 1.0, (), jnp.float32)
    in_im = gaussian(key_list[8], (GROUPS_S5, STATE, GROUP_CH), (2 * GROUP_CH) ** -0.5, 1.0, (), jnp.float32)
    out_re = gaussian(key_list[9], (GROUPS_S5, GROUP_CH, STATE), STATE ** -0.5, 0.75, (), jnp.float32)
    out_im = gaussian(key_list[10], (GROUPS_S5, GROUP_CH, STATE), STATE ** -0.5, 0.75, (), jnp.float32)
    skip = gaussian(key_list[11], (S5W,), 1.0, 4.0, (), jnp.float32)
    w_glu = gaussian(key_list[12], (S5W, S5W), S5W ** -0.5, 0.1875)
    w_out = gaussian(key_list[13], (S5W, D), (S5W // 4) ** -0.5, 0.375)
    ffn_gain = jnp.clip(1.0 + 0.18 * jax.random.normal(key_list[14], (D,), jnp.float32), 0.1, 1.9)
    w_group = gaussian(key_list[15], (D, EXP_GROUPS), (16 * D) ** -0.5, 0.03125)
    w_route = gaussian(key_list[16], (D, EXPERTS), (16 * D) ** -0.5, 0.03125)
    w_gate = gaussian(key_list[17], (EXPERTS, D, FFE), D ** -0.5, 0.125, ((0, 16),))
    w_up = gaussian(key_list[18], (EXPERTS, D, FFE), D ** -0.5, 0.125, ((0, 16),))
    w_down = gaussian(key_list[19], (EXPERTS, FFE, D), (max(FFE // 64, 1)) ** -0.5, 2.0, ((0, 16),))
    route_ids = draw_route_ids(jax.random.fold_in(jax.random.fold_in(key_list[21], part), 71), part)
    return dict(hidden=hidden, state=state, norm_gain=norm_gain, w_in=w_in, lam_re=lam_re, lam_im=lam_im, log_step=log_step, in_re=in_re, in_im=in_im, out_re=out_re, out_im=out_im, skip=skip, w_glu=w_glu, w_out=w_out, ffn_gain=ffn_gain, w_group=w_group, w_route=w_route, w_gate=w_gate, w_up=w_up, w_down=w_down, route_ids=route_ids)


def normalize(rows, gain):
    wide = rows.astype(jnp.float32)
    return wide * lax.rsqrt(lax.optimization_barrier(jnp.mean(wide * wide, axis=-1, keepdims=True)) + 1e-06) * gain

def discretize(lam_re, lam_im, log_step, in_re, in_im):
    step = jnp.exp(log_step)[:, None]
    magnitude = jnp.exp(lam_re * step)
    bar_re = magnitude * jnp.cos(lam_im * step)
    bar_im = magnitude * jnp.sin(lam_im * step)
    denom = lam_re * lam_re + lam_im * lam_im
    lessened = bar_re - 1.0
    coef_re = (lessened * lam_re + bar_im * lam_im) / denom
    coef_im = (bar_im * lam_re - lessened * lam_im) / denom
    drive_re = coef_re[:, :, None] * in_re - coef_im[:, :, None] * in_im
    drive_im = coef_re[:, :, None] * in_im + coef_im[:, :, None] * in_re
    return (bar_re, bar_im, drive_re, drive_im)

def mixer_step(inputs, state, lam_re, lam_im, log_step, in_re, in_im, out_re, out_im, skip, w_glu):
    rows = inputs.shape[0]
    groups, entries = lam_re.shape
    width = in_re.shape[2]
    highest = lax.Precision.HIGHEST
    bar_re, bar_im, drive_re, drive_im = discretize(lam_re, lam_im, log_step, in_re, in_im)
    wide = inputs.astype(jnp.float32)
    grouped = wide.reshape(rows, groups, width)
    push_re = jnp.einsum('bgc,gnc->bgn', grouped, drive_re, precision=highest)
    push_im = jnp.einsum('bgc,gnc->bgn', grouped, drive_im, precision=highest)
    old_re = state[0].reshape(rows, groups, entries)
    old_im = state[1].reshape(rows, groups, entries)
    new_re = bar_re * old_re - bar_im * old_im + push_re
    new_im = bar_re * old_im + bar_im * old_re + push_im
    read = jnp.einsum('bgn,gcn->bgc', new_re, out_re, precision=highest) - jnp.einsum('bgn,gcn->bgc', new_im, out_im, precision=highest)
    mixed = read.reshape(rows, groups * width) + skip * wide
    active = jax.nn.gelu(mixed)
    gating = jnp.dot(active.astype(jnp.bfloat16), w_glu, preferred_element_type=jnp.float32)
    result = (active * jax.nn.sigmoid(gating)).astype(jnp.bfloat16)
    new_state = jnp.stack([new_re.reshape(rows, -1), new_im.reshape(rows, -1)])
    return (result, new_state)

def route_gates(normed, w_group, w_route, route_ids, per_group):
    group_logit = jnp.dot(normed, w_group, preferred_element_type=jnp.float32)
    route_logit = jnp.dot(normed, w_route, preferred_element_type=jnp.float32)
    chosen = route_ids[:, 0] // per_group
    pick_group = (chosen[:, None] == jnp.arange(group_logit.shape[1], dtype=jnp.int32)[None, :]).astype(jnp.float32)
    own = lax.optimization_barrier(jnp.sum(group_logit * pick_group, axis=1, keepdims=True))
    group_weight = 1.0 / lax.optimization_barrier(jnp.sum(jnp.exp(group_logit - own), axis=1))
    pick = (route_ids[:, :, None] == jnp.arange(route_logit.shape[1], dtype=jnp.int32)[None, None, :]).astype(jnp.float32)
    chosen_logit = lax.optimization_barrier(jnp.sum(pick * route_logit[:, None, :], axis=2))
    first = jax.nn.sigmoid(chosen_logit[:, 0] - chosen_logit[:, 1])
    pair = jnp.stack([first, 1.0 - first], axis=1)
    return group_weight[:, None] * pair

def reference(hidden, state, norm_gain, w_in, lam_re, lam_im, log_step, in_re, in_im, out_re, out_im, skip, w_glu, w_out, ffn_gain, w_group, w_route, w_gate, w_up, w_down, route_ids):
    normed = normalize(hidden, norm_gain).astype(jnp.bfloat16)
    inputs = jnp.dot(normed, w_in, preferred_element_type=jnp.float32).astype(jnp.bfloat16)
    glu, new_state = mixer_step(inputs, state, lam_re, lam_im, log_step, in_re, in_im, out_re, out_im, skip, w_glu)
    resid = (hidden.astype(jnp.float32) + jnp.dot(glu, w_out, preferred_element_type=jnp.float32)).astype(jnp.bfloat16)
    normed2 = normalize(resid, ffn_gain).astype(jnp.bfloat16)
    gates = route_gates(normed2, w_group, w_route, route_ids, EPG)
    limit = N_EP * CAP

    def visit(total, expert):
        hit = route_ids == expert
        weight = lax.optimization_barrier(jnp.sum(jnp.where(hit, gates, 0.0), axis=1))
        used = jnp.any(hit, axis=1)
        count = jnp.sum(used.astype(jnp.int32))
        index = jnp.nonzero(used, size=limit, fill_value=0)[0].astype(jnp.int32)
        valid = (jnp.arange(limit, dtype=jnp.int32) < count).astype(jnp.float32)
        rows = normed2[index]
        gate = jnp.dot(rows, w_gate[expert], preferred_element_type=jnp.float32)
        upper = jnp.dot(rows, w_up[expert], preferred_element_type=jnp.float32)
        inner = (jax.nn.silu(gate) * upper).astype(jnp.bfloat16)
        result = jnp.dot(inner, w_down[expert], preferred_element_type=jnp.float32).astype(jnp.bfloat16)
        scale = weight[index] * valid
        total = total.at[index].add(scale[:, None] * result.astype(jnp.float32))
        return (total, None)
    start = jnp.zeros((hidden.shape[0], hidden.shape[1]), jnp.float32)
    total, unused = lax.scan(visit, start, jnp.arange(EXPERTS, dtype=jnp.int32))
    hidden_out = (resid.astype(jnp.float32) + total).astype(jnp.bfloat16)
    return (hidden_out, new_state)
```

```python
import functools

import jax
import jax.numpy as jnp
from jax import lax
from jax.experimental import pallas as pl
from jax.experimental.pallas import tpu as pltpu
from jax.sharding import PartitionSpec as P

EXP_GROUPS = 4
TOPK = 2
QUAD = 4


def normalize(rows, gain):
    wide = rows.astype(jnp.float32)
    return wide * lax.rsqrt(jnp.mean(wide * wide, axis=-1, keepdims=True) + 1e-06) * gain


def discretize(lam_re, lam_im, log_step, in_re, in_im):
    step = jnp.exp(log_step)[:, None]
    magnitude = jnp.exp(lam_re * step)
    bar_re = magnitude * jnp.cos(lam_im * step)
    bar_im = magnitude * jnp.sin(lam_im * step)
    denom = lam_re * lam_re + lam_im * lam_im
    lessened = bar_re - 1.0
    coef_re = ((lessened * lam_re + bar_im * lam_im) / denom)[:, None, :]
    coef_im = ((bar_im * lam_re - lessened * lam_im) / denom)[:, None, :]
    in_re = in_re.transpose(0, 2, 1)
    in_im = in_im.transpose(0, 2, 1)
    drive_re = coef_re * in_re - coef_im * in_im
    drive_im = coef_re * in_im + coef_im * in_re
    return (bar_re, bar_im, drive_re, drive_im)


def split(wide):
    high = wide.astype(jnp.bfloat16)
    return high, (wide - high.astype(jnp.float32)).astype(jnp.bfloat16)


def dot(a, b):
    return jnp.dot(a, b, preferred_element_type=jnp.float32)


def dot_t(a, b):
    return lax.dot_general(a, b, (((1,), (1,)), ((), ())), preferred_element_type=jnp.float32)


def mixer_kernel(
    u_ref,
    state_ref,
    bar_ref,
    dre_ref,
    dim_ref,
    ore_ref,
    oim_ref,
    skip_ref,
    hidden_ref,
    gain_ref,
    router_ref,
    dispatch_ref,
    w_glu_ref,
    w_out_ref,
    new_ref,
    resid_ref,
    outgoing_ref,
    logits_ref,
    active_ref,
    glu_v,
    out_v,
    sems,
    *,
    width,
    entries,
):
    at = pl.program_id(0)
    last = pl.num_programs(0) - 1
    copy_glu = pltpu.make_async_copy(w_glu_ref, glu_v, sems.at[0])
    copy_out = pltpu.make_async_copy(w_out_ref, out_v, sems.at[1])

    @pl.when(at == 0)
    def _():
        copy_glu.start()
        copy_out.start()

    chans = u_ref.shape[1]
    lanes = state_ref.shape[2]
    row_group = lax.broadcasted_iota(jnp.int32, (chans, lanes), 0) // width
    lane_group = lax.broadcasted_iota(jnp.int32, (chans, lanes), 1) // entries
    same = row_group == lane_group

    def spread(ref):
        piece = ref[...]
        return jnp.where(same, jnp.concatenate([piece] * (lanes // piece.shape[1]), axis=1), 0.0)

    u = u_ref[...]
    drive_hi, drive_lo = split(jnp.concatenate([spread(dre_ref), spread(dim_ref)], axis=1))
    push = dot(jnp.concatenate([u, u], axis=1), jnp.concatenate([drive_hi, drive_lo], axis=0))
    bar_re = bar_ref[0:1, :]
    bar_im = bar_ref[1:2, :]
    old_re = state_ref[0]
    old_im = state_ref[1]
    new_re = bar_re * old_re - bar_im * old_im + push[:, :lanes]
    new_im = bar_re * old_im + bar_im * old_re + push[:, lanes:]
    new_ref[0] = new_re
    new_ref[1] = new_im
    new_hi, new_lo = split(jnp.concatenate([new_re, new_im], axis=1))
    read_hi, read_lo = split(jnp.concatenate([spread(ore_ref), -spread(oim_ref)], axis=1))
    read = dot_t(new_hi, read_hi) + dot_t(new_lo, read_hi) + dot_t(new_hi, read_lo)
    mixed = read + skip_ref[...] * u.astype(jnp.float32)
    active_ref[:, pl.ds(pl.multiple_of(at * chans, chans), chans)] = jax.nn.gelu(mixed)

    @pl.when(at == last)
    def _():
        copy_glu.wait()
        active = active_ref[...]
        gating = dot(active.astype(jnp.bfloat16), glu_v[...])
        glu = (active * jax.nn.sigmoid(gating)).astype(jnp.bfloat16)
        copy_out.wait()
        resid = (hidden_ref[...].astype(jnp.float32) + dot(glu, out_v[...])).astype(jnp.bfloat16)
        resid_ref[...] = resid
        normed = normalize(resid, gain_ref[...]).astype(jnp.bfloat16)
        outgoing_ref[...] = dot(dispatch_ref[...], normed).astype(jnp.bfloat16)
        logits_ref[...] = dot(normed, router_ref[...])


def mixer(u, state, bar, dre, dim, ore, oim, skip, hidden, gain, router, dispatch, w_glu, w_out, width, entries):
    rows, channels = u.shape
    chans = min(128, channels)
    steps = channels // chans
    lanes = chans // width * entries
    model = hidden.shape[1]

    def whole(a):
        return pl.BlockSpec(a.shape, lambda i: (0,) * a.ndim)

    along = pl.BlockSpec((chans, dre.shape[1]), lambda i: (i, 0))
    states = pl.BlockSpec((2, rows, lanes), lambda i: (0, 0, i))
    out_shape = (
        jax.ShapeDtypeStruct(state.shape, jnp.float32),
        jax.ShapeDtypeStruct(hidden.shape, jnp.bfloat16),
        jax.ShapeDtypeStruct((dispatch.shape[0], model), jnp.bfloat16),
        jax.ShapeDtypeStruct((rows, router.shape[1]), jnp.float32),
    )
    return pl.pallas_call(
        functools.partial(mixer_kernel, width=width, entries=entries),
        grid=(steps,),
        in_specs=[
            pl.BlockSpec((rows, chans), lambda i: (0, i)),
            states,
            pl.BlockSpec((2, lanes), lambda i: (0, i)),
            along,
            along,
            along,
            along,
            pl.BlockSpec((1, chans), lambda i: (0, i)),
            whole(hidden),
            whole(gain),
            whole(router),
            whole(dispatch),
            pl.BlockSpec(memory_space=pl.ANY),
            pl.BlockSpec(memory_space=pl.ANY),
        ],
        out_specs=(states,) + tuple(whole(s) for s in out_shape[1:]),
        out_shape=out_shape,
        scratch_shapes=[
            pltpu.VMEM((rows, channels), jnp.float32),
            pltpu.VMEM(w_glu.shape, w_glu.dtype),
            pltpu.VMEM(w_out.shape, w_out.dtype),
            pltpu.SemaphoreType.DMA((2,)),
        ],
        name="mixer",
    )(u, state, bar, dre, dim, ore, oim, skip, hidden, gain, router, dispatch, w_glu, w_out)


def combine_kernel(slot_ref, gates_ref, resid_ref, returned_ref, out_ref):
    slots = returned_ref.shape[0]
    rows = resid_ref.shape[0]
    lane = lax.broadcasted_iota(jnp.int32, (rows, slots), 1)
    weight = jnp.zeros((rows, slots), jnp.float32)
    for k in range(TOPK):
        weight = weight + jnp.where(slot_ref[:, k : k + 1] == lane, gates_ref[:, k : k + 1], 0.0)
    high, low = split(weight)
    returned = returned_ref[...]
    moe = dot(high, returned) + dot(low, returned)
    out_ref[...] = (resid_ref[...].astype(jnp.float32) + moe).astype(jnp.bfloat16)


def combine(slot, gates, resid, returned):
    model = resid.shape[1]
    piece = min(512, model)

    def column(a):
        return pl.BlockSpec((a.shape[0], piece), lambda i: (0, i))

    def whole(a):
        return pl.BlockSpec(a.shape, lambda i: (0, 0))

    return pl.pallas_call(
        combine_kernel,
        grid=(model // piece,),
        in_specs=[whole(slot), whole(gates), column(resid), column(returned)],
        out_specs=column(resid),
        out_shape=jax.ShapeDtypeStruct(resid.shape, jnp.bfloat16),
        name="combine",
    )(slot, gates, resid, returned)


def route_gates(group_logit, route_logit, route_ids, per_group):
    chosen = route_ids[:, 0] // per_group
    pick_group = (
        chosen[:, None] == jnp.arange(group_logit.shape[1], dtype=jnp.int32)[None, :]
    ).astype(jnp.float32)
    own = jnp.sum(group_logit * pick_group, axis=1, keepdims=True)
    group_weight = 1.0 / jnp.sum(jnp.exp(group_logit - own), axis=1)
    pick = (
        route_ids[:, :, None] == jnp.arange(route_logit.shape[1], dtype=jnp.int32)[None, None, :]
    ).astype(jnp.float32)
    chosen_logit = jnp.sum(pick * route_logit[:, None, :], axis=2)
    first = jax.nn.sigmoid(chosen_logit[:, 0] - chosen_logit[:, 1])
    pair = jnp.stack([first, 1.0 - first], axis=1)
    return group_weight[:, None] * pair


def project(normed, w_in):
    ranks = lax.axis_size("ep")
    me = lax.axis_index("ep")
    quads = ranks // QUAD
    rows = normed.shape[0]
    shard = w_in.shape[1]

    def across(a, k):
        return lax.ppermute(a, "ep", [(r, r ^ k) for r in range(ranks)])

    own = w_in.T
    shards = [own] + [
        lax.ppermute(own, "ep", [(r, (r + QUAD * d) % ranks) for r in range(ranks)])
        for d in range(1, quads)
    ]
    far = across(normed, 2)
    near = across(jnp.concatenate([normed, far], axis=0), 1)
    tokens = jnp.concatenate([normed, far, near], axis=0)
    table = jnp.concatenate(shards, axis=0)
    partial = dot_t(tokens, table).astype(jnp.bfloat16)
    order = (0, 2, 1, 3)
    pieces = [partial[:rows]] + [
        across(partial[i * rows : (i + 1) * rows], order[i]) for i in range(1, QUAD)
    ]
    joined = jnp.concatenate(pieces, axis=1)
    total = ranks * shard
    source = jnp.arange(total, dtype=jnp.int32)
    which, offset, inside = source // (quads * shard), source // shard % quads, source % shard
    k = jnp.where(which == 1, 2, jnp.where(which == 2, 1, which))
    rank = (me // QUAD - offset) % quads * QUAD + ((me % QUAD) ^ k)
    target = rank * shard + inside
    turn = (target[:, None] == jnp.arange(total, dtype=jnp.int32)[None, :]).astype(jnp.bfloat16)
    return dot(joined, turn).astype(jnp.bfloat16)


def on_device(
    hidden,
    state,
    norm_gain,
    w_in,
    lam_re,
    lam_im,
    log_step,
    in_re,
    in_im,
    out_re,
    out_im,
    skip,
    w_glu,
    w_out,
    ffn_gain,
    w_group,
    w_route,
    w_gate,
    w_up,
    w_down,
    route_ids,
):
    groups, entries = lam_re.shape
    width = in_re.shape[2]
    count_dev, model_width = hidden.shape
    experts = w_route.shape[1]
    sources = lax.axis_size("ep")
    normed = normalize(hidden, norm_gain).astype(jnp.bfloat16)
    inputs = project(normed, w_in)

    bar_re, bar_im, drive_re, drive_im = discretize(lam_re, lam_im, log_step, in_re, in_im)
    bar = jnp.stack([bar_re.reshape(-1), bar_im.reshape(-1)])
    copies = max(1, 128 // entries)

    def lined(a):
        return jnp.tile(a.reshape(groups * width, entries), (1, copies))

    capacity = 2 * TOPK * count_dev // experts
    flat = route_ids.reshape(-1)
    hits = (flat[:, None] == jnp.arange(experts, dtype=jnp.int32)[None, :]).astype(jnp.int32)
    before = jnp.sum((jnp.cumsum(hits, axis=0) - hits) * hits, axis=1)
    slot = (flat * capacity + before).reshape(count_dev, TOPK)
    lane = jnp.arange(experts * capacity, dtype=jnp.int32)
    dispatch = jnp.any(slot.T[:, None, :] == lane[None, :, None], axis=0).astype(jnp.bfloat16)
    router = jnp.concatenate([w_group, w_route], axis=1)
    used = router.shape[1]
    router = jnp.pad(router, ((0, 0), (0, -used % 128)))

    new_state, resid, outgoing, logits = mixer(
        inputs,
        state,
        bar,
        lined(drive_re),
        lined(drive_im),
        lined(out_re),
        lined(out_im),
        skip[None, :],
        hidden,
        ffn_gain[None, :],
        router,
        dispatch,
        w_glu,
        w_out,
        width,
        entries,
    )
    received = lax.all_to_all(
        outgoing.reshape(experts, capacity, model_width), "ep", split_axis=0, concat_axis=0, tiled=True
    )
    arranged = received.reshape(experts * capacity, model_width)
    gate = dot(arranged, w_gate[0])
    upper = dot(arranged, w_up[0])
    inner = (jax.nn.silu(gate) * upper).astype(jnp.bfloat16)
    result = dot(inner, w_down[0]).astype(jnp.bfloat16)
    returned = lax.all_to_all(
        result.reshape(sources, capacity, model_width), "ep", split_axis=0, concat_axis=0, tiled=True
    )
    groups_used = w_group.shape[1]
    gates = route_gates(
        logits[:, :groups_used], logits[:, groups_used:used], route_ids, experts // EXP_GROUPS
    )
    hidden_out = combine(slot, gates, resid, returned.reshape(experts * capacity, model_width))
    return (hidden_out, new_state)


def solution(mesh):
    return jax.shard_map(
        on_device,
        mesh=mesh,
        in_specs=(
            P(("grp", "ep"), None),
            P(None, ("grp", "ep"), None),
            P(),
            P(None, "ep"),
            P(),
            P(),
            P(),
            P(),
            P(),
            P(),
            P(),
            P(),
            P(),
            P(),
            P(),
            P(),
            P(),
            P("ep", None, None),
            P("ep", None, None),
            P("ep", None, None),
            P(("grp", "ep"), None),
        ),
        out_specs=(P(("grp", "ep"), None), P(None, ("grp", "ep"), None)),
        check_vma=False,
    )
```

```python
import functools

import jax
import jax.numpy as jnp
from jax import lax
from jax.experimental import pallas as pl
from jax.experimental.pallas import tpu as pltpu
from jax.sharding import PartitionSpec as P

EXP_GROUPS = 4
TOPK = 2
QUAD = 4


def normalize(rows, gain):
    wide = rows.astype(jnp.float32)
    return wide * lax.rsqrt(jnp.mean(wide * wide, axis=-1, keepdims=True) + 1e-06) * gain


def discretize(lam_re, lam_im, log_step, in_re, in_im):
    step = jnp.exp(log_step)[:, None]
    magnitude = jnp.exp(lam_re * step)
    bar_re = magnitude * jnp.cos(lam_im * step)
    bar_im = magnitude * jnp.sin(lam_im * step)
    denom = lam_re * lam_re + lam_im * lam_im
    lessened = bar_re - 1.0
    coef_re = ((lessened * lam_re + bar_im * lam_im) / denom)[:, None, :]
    coef_im = ((bar_im * lam_re - lessened * lam_im) / denom)[:, None, :]
    in_re = in_re.transpose(0, 2, 1)
    in_im = in_im.transpose(0, 2, 1)
    drive_re = coef_re * in_re - coef_im * in_im
    drive_im = coef_re * in_im + coef_im * in_re
    return (bar_re, bar_im, drive_re, drive_im)


def split(wide):
    high = wide.astype(jnp.bfloat16)
    return high, (wide - high.astype(jnp.float32)).astype(jnp.bfloat16)


def dot(a, b):
    return jnp.dot(a, b, preferred_element_type=jnp.float32)


def dot_t(a, b):
    return lax.dot_general(a, b, (((1,), (1,)), ((), ())), preferred_element_type=jnp.float32)


def mixer_kernel(
    u_ref,
    state_ref,
    bar_ref,
    dre_ref,
    dim_ref,
    ore_ref,
    oim_ref,
    skip_ref,
    hidden_ref,
    gain_ref,
    dispatch_ref,
    w_glu_ref,
    w_out_ref,
    new_ref,
    resid_ref,
    outgoing_ref,
    normed_ref,
    active_ref,
    glu_v,
    out_v,
    same_ref,
    sems,
    *,
    width,
    entries,
):
    at = pl.program_id(0)
    last = pl.num_programs(0) - 1
    copy_glu = pltpu.make_async_copy(w_glu_ref, glu_v, sems.at[0])
    copy_out = pltpu.make_async_copy(w_out_ref, out_v, sems.at[1])

    @pl.when(at == 0)
    def _():
        copy_glu.start()
        copy_out.start()

    chans = u_ref.shape[1]
    lanes = state_ref.shape[2]

    @pl.when(at == 0)
    def _():
        row_group = lax.broadcasted_iota(jnp.int32, (chans, lanes), 0) // width
        lane_group = lax.broadcasted_iota(jnp.int32, (chans, lanes), 1) // entries
        same_ref[...] = (row_group == lane_group).astype(jnp.float32).astype(jnp.bfloat16)

    same = same_ref[...]

    def spread(ref):
        piece = ref[...]
        twice = split(jnp.concatenate([piece, piece], axis=1))
        return [jnp.concatenate([h] * (lanes // h.shape[1]), axis=1) * same for h in twice]

    u = u_ref[...]
    drive = [jnp.concatenate(pair, axis=1) for pair in zip(spread(dre_ref), spread(dim_ref))]
    push = dot(jnp.concatenate([u, u], axis=1), jnp.concatenate(drive, axis=0))
    bar_re = bar_ref[0:1, :]
    bar_im = bar_ref[1:2, :]
    old_re = state_ref[0]
    old_im = state_ref[1]
    new_re = bar_re * old_re - bar_im * old_im + push[:, :lanes]
    new_im = bar_re * old_im + bar_im * old_re + push[:, lanes:]
    new_ref[0] = new_re
    new_ref[1] = new_im
    new_hi, new_lo = split(jnp.concatenate([new_re, new_im], axis=1))
    read_hi, read_lo = [
        jnp.concatenate([real, -imag], axis=1) for real, imag in zip(spread(ore_ref), spread(oim_ref))
    ]
    read = dot_t(new_hi, read_hi) + dot_t(new_lo, read_hi) + dot_t(new_hi, read_lo)
    mixed = read + skip_ref[...] * u.astype(jnp.float32)
    active_ref[:, pl.ds(pl.multiple_of(at * chans, chans), chans)] = jax.nn.gelu(mixed)

    @pl.when(at == last)
    def _():
        copy_glu.wait()
        active = active_ref[...]
        gating = dot(active.astype(jnp.bfloat16), glu_v[...])
        glu = (active * jax.nn.sigmoid(gating)).astype(jnp.bfloat16)
        copy_out.wait()
        resid = (hidden_ref[...].astype(jnp.float32) + dot(glu, out_v[...])).astype(jnp.bfloat16)
        resid_ref[...] = resid
        normed = normalize(resid, gain_ref[...]).astype(jnp.bfloat16)
        outgoing_ref[...] = dot(dispatch_ref[...], normed).astype(jnp.bfloat16)
        normed_ref[...] = normed


def mixer(u, state, bar, dre, dim, ore, oim, skip, hidden, gain, dispatch, w_glu, w_out, width, entries):
    rows, channels = u.shape
    chans = min(128, channels)
    steps = channels // chans
    lanes = chans // width * entries
    model = hidden.shape[1]

    def whole(a):
        return pl.BlockSpec(a.shape, lambda i: (0,) * a.ndim)

    along = pl.BlockSpec((chans, dre.shape[1]), lambda i: (i, 0))
    states = pl.BlockSpec((2, rows, lanes), lambda i: (0, 0, i))
    out_shape = (
        jax.ShapeDtypeStruct(state.shape, jnp.float32),
        jax.ShapeDtypeStruct(hidden.shape, jnp.bfloat16),
        jax.ShapeDtypeStruct((dispatch.shape[0], model), jnp.bfloat16),
        jax.ShapeDtypeStruct(hidden.shape, jnp.bfloat16),
    )
    return pl.pallas_call(
        functools.partial(mixer_kernel, width=width, entries=entries),
        grid=(steps,),
        in_specs=[
            pl.BlockSpec((rows, chans), lambda i: (0, i)),
            states,
            pl.BlockSpec((2, lanes), lambda i: (0, i)),
            along,
            along,
            along,
            along,
            pl.BlockSpec((1, chans), lambda i: (0, i)),
            whole(hidden),
            whole(gain),
            whole(dispatch),
            pl.BlockSpec(memory_space=pl.ANY),
            pl.BlockSpec(memory_space=pl.ANY),
        ],
        out_specs=(states,) + tuple(whole(s) for s in out_shape[1:]),
        out_shape=out_shape,
        scratch_shapes=[
            pltpu.VMEM((rows, channels), jnp.float32),
            pltpu.VMEM(w_glu.shape, w_glu.dtype),
            pltpu.VMEM(w_out.shape, w_out.dtype),
            pltpu.VMEM((chans, lanes), jnp.bfloat16),
            pltpu.SemaphoreType.DMA((2,)),
        ],
        name="mixer",
    )(u, state, bar, dre, dim, ore, oim, skip, hidden, gain, dispatch, w_glu, w_out)


def combine_kernel(slot_ref, gates_ref, resid_ref, returned_ref, out_ref, high_ref, low_ref):
    slots = returned_ref.shape[0]
    rows = resid_ref.shape[0]

    @pl.when(pl.program_id(0) == 0)
    def _():
        lane = lax.broadcasted_iota(jnp.int32, (rows, slots), 1)
        weight = jnp.zeros((rows, slots), jnp.float32)
        for k in range(TOPK):
            weight = weight + jnp.where(slot_ref[:, k : k + 1] == lane, gates_ref[:, k : k + 1], 0.0)
        high_ref[...], low_ref[...] = split(weight)

    returned = returned_ref[...]
    moe = dot(high_ref[...], returned) + dot(low_ref[...], returned)
    out_ref[...] = (resid_ref[...].astype(jnp.float32) + moe).astype(jnp.bfloat16)


def combine(slot, gates, resid, returned):
    model = resid.shape[1]
    piece = min(512, model)

    def column(a):
        return pl.BlockSpec((a.shape[0], piece), lambda i: (0, i))

    def whole(a):
        return pl.BlockSpec(a.shape, lambda i: (0, 0))

    return pl.pallas_call(
        combine_kernel,
        grid=(model // piece,),
        in_specs=[whole(slot), whole(gates), column(resid), column(returned)],
        out_specs=column(resid),
        out_shape=jax.ShapeDtypeStruct(resid.shape, jnp.bfloat16),
        scratch_shapes=[pltpu.VMEM((resid.shape[0], returned.shape[0]), jnp.bfloat16)] * 2,
        name="combine",
    )(slot, gates, resid, returned)


def route_gates(group_logit, route_logit, route_ids, per_group):
    chosen = route_ids[:, 0] // per_group
    pick_group = (
        chosen[:, None] == jnp.arange(group_logit.shape[1], dtype=jnp.int32)[None, :]
    ).astype(jnp.float32)
    own = jnp.sum(group_logit * pick_group, axis=1, keepdims=True)
    group_weight = 1.0 / jnp.sum(jnp.exp(group_logit - own), axis=1)
    pick = (
        route_ids[:, :, None] == jnp.arange(route_logit.shape[1], dtype=jnp.int32)[None, None, :]
    ).astype(jnp.float32)
    chosen_logit = jnp.sum(pick * route_logit[:, None, :], axis=2)
    first = jax.nn.sigmoid(chosen_logit[:, 0] - chosen_logit[:, 1])
    pair = jnp.stack([first, 1.0 - first], axis=1)
    return group_weight[:, None] * pair


def project(normed, w_in):
    ranks = lax.axis_size("ep")
    me = lax.axis_index("ep")
    quads = ranks // QUAD
    rows = normed.shape[0]
    shard = w_in.shape[1]

    def across(a, k):
        return lax.ppermute(a, "ep", [(r, r ^ k) for r in range(ranks)])

    own = w_in.T
    near = across(normed, 1)
    far = across(normed, 2)
    shards = [own]
    for d in range(1, quads):
        shards += [lax.ppermute(own, "ep", [(r, (r + QUAD * d) % ranks) for r in range(ranks)])]
    tokens = jnp.concatenate([normed, near, far, across(far, 1)], axis=0)
    table = jnp.concatenate(shards, axis=0)
    partial = dot_t(tokens, table).astype(jnp.bfloat16)
    pieces = [partial[:rows]] + [
        across(partial[i * rows : (i + 1) * rows], i) for i in range(1, QUAD)
    ]
    joined = jnp.concatenate(pieces, axis=1)
    total = ranks * shard
    source = jnp.arange(total, dtype=jnp.int32)
    which, offset, inside = source // (quads * shard), source // shard % quads, source % shard
    rank = (me // QUAD - offset) % quads * QUAD + ((me % QUAD) ^ which)
    target = rank * shard + inside
    turn = (target[:, None] == jnp.arange(total, dtype=jnp.int32)[None, :]).astype(jnp.bfloat16)
    return dot(joined, turn).astype(jnp.bfloat16)


def on_device(
    hidden,
    state,
    norm_gain,
    w_in,
    lam_re,
    lam_im,
    log_step,
    in_re,
    in_im,
    out_re,
    out_im,
    skip,
    w_glu,
    w_out,
    ffn_gain,
    w_group,
    w_route,
    w_gate,
    w_up,
    w_down,
    route_ids,
):
    groups, entries = lam_re.shape
    width = in_re.shape[2]
    count_dev, model_width = hidden.shape
    experts = w_route.shape[1]
    sources = lax.axis_size("ep")
    normed = normalize(hidden, norm_gain).astype(jnp.bfloat16)
    inputs = project(normed, w_in)

    bar_re, bar_im, drive_re, drive_im = discretize(lam_re, lam_im, log_step, in_re, in_im)
    bar = jnp.stack([bar_re.reshape(-1), bar_im.reshape(-1)])

    def lined(a):
        return a.reshape(groups * width, entries)

    capacity = 2 * TOPK * count_dev // experts
    flat = route_ids.reshape(-1)
    hits = (flat[:, None] == jnp.arange(experts, dtype=jnp.int32)[None, :]).astype(jnp.int32)
    before = jnp.sum((jnp.cumsum(hits, axis=0) - hits) * hits, axis=1)
    slot = (flat * capacity + before).reshape(count_dev, TOPK)
    lane = jnp.arange(experts * capacity, dtype=jnp.int32)
    dispatch = jnp.any(slot.T[:, None, :] == lane[None, :, None], axis=0).astype(jnp.bfloat16)

    new_state, resid, outgoing, normed2 = mixer(
        inputs,
        state,
        bar,
        lined(drive_re),
        lined(drive_im),
        lined(out_re),
        lined(out_im),
        skip[None, :],
        hidden,
        ffn_gain[None, :],
        dispatch,
        w_glu,
        w_out,
        width,
        entries,
    )
    received = lax.all_to_all(
        outgoing.reshape(experts, capacity, model_width), "ep", split_axis=0, concat_axis=0, tiled=True
    )
    arranged = received.reshape(experts * capacity, model_width)
    gate = dot(arranged, w_gate[0])
    upper = dot(arranged, w_up[0])
    inner = lax.optimization_barrier((jax.nn.silu(gate) * upper).astype(jnp.bfloat16))
    result = dot(inner, w_down[0]).astype(jnp.bfloat16)
    returned = lax.all_to_all(
        result.reshape(sources, capacity, model_width), "ep", split_axis=0, concat_axis=0, tiled=True
    )
    gates = route_gates(dot(normed2, w_group), dot(normed2, w_route), route_ids, experts // EXP_GROUPS)
    hidden_out = combine(slot, gates, resid, returned.reshape(experts * capacity, model_width))
    return (hidden_out, new_state)


def solution(mesh):
    return jax.shard_map(
        on_device,
        mesh=mesh,
        in_specs=(
            P(("grp", "ep"), None),
            P(None, ("grp", "ep"), None),
            P(),
            P(None, "ep"),
            P(),
            P(),
            P(),
            P(),
            P(),
            P(),
            P(),
            P(),
            P(),
            P(),
            P(),
            P(),
            P(),
            P("ep", None, None),
            P("ep", None, None),
            P("ep", None, None),
            P(("grp", "ep"), None),
        ),
        out_specs=(P(("grp", "ep"), None), P(None, ("grp", "ep"), None)),
        check_vma=False,
    )
```
